32 devices in a mesh: sp: 8 (over z, y), tp: 4 (over x, core).
Axes of the slice: x: 2, y: 2, z: 4, core: 2. Of those that a mesh axis runs over, the one named last changes fastest.
Arguments:
- tokens: bfloat16 [8192, 2048], P('sp'), may hold values from -6 to 6
- norm_gain: float32 [2048], replicated, may hold values from 0.1 to 1.9
- w_query: bfloat16 [2048, 1024], P('sp', 'tp'), may hold values from -3.5 to 3.5
- w_key: bfloat16 [2048, 256], P('sp', 'tp'), may hold values from -0.125 to 0.125
- w_value: bfloat16 [2048, 256], P('sp', 'tp'), may hold values from -0.125 to 0.125
- w_content: bfloat16 [2048, 1024], P('sp', 'tp'), may hold values from -0.125 to 0.125
- w_gate: bfloat16 [2048, 1024], P('sp', 'tp'), may hold values from -0.125 to 0.125
- sink_logit: float32 [16], P('tp'), may hold values from 1 to 6
- conv_weight: float32 [31, 1024], P(None, 'tp'), may hold values from -10 to 10
- conv_bias: float32 [1024], P('tp'), may hold values from 0 to 20
- channel_gain: float32 [1024], P('tp'), may hold values from 0.1 to 1.9
- out_attn: bfloat16 [1024, 2048], P('tp', 'sp'), may hold values from -0.75 to 0.75
- out_conv: bfloat16 [1024, 2048], P('tp', 'sp'), may hold values from -0.1875 to 0.1875
Outputs:
- mixed: bfloat16 [8192, 2048], P(('sp', 'tp'))
The draws below stay inside these ranges and needn't reach their ends.
All inputs are finite; a program needn't handle non-finite values.
Results may differ from the reference program's by a relative error of at most 0.025.
The reference program's roundings to bfloat16 on the way count: a program that leaves them out, or rounds other values in their place, can miss the bound.
Values may be sent and summed in bfloat16 or wider, within the bound.
A program may use at most 64 MiB of HBM per device.

```python
import math
import jax
import jax.numpy as jnp
from jax import lax

D = 2048
HEADS = 16
KV_HEADS = 4
HEAD_DIM = 64
CONV_CH = 1024
KERNEL = 31
WINDOW = 128
TOKENS = 8192
ATTN_W = 1024
N_TP = 4


def draw_w_query(key, part):
    normal_part = jax.random.normal(key, (D, HEADS * HEAD_DIM), jnp.float32)
    return jnp.clip(normal_part / math.sqrt(D), -3.5, 3.5).astype(jnp.bfloat16)


def draw_conv_weight(key, part):
    normal_key = jax.random.fold_in(key, 11)
    jitter_key = jax.random.fold_in(key, 12)
    normal_part = jnp.clip(jax.random.normal(normal_key, (KERNEL, CONV_CH), jnp.float32), -4.0, 4.0)
    channel_ramp = jnp.arange(CONV_CH, dtype=jnp.float32) / CONV_CH
    jitter = jax.random.uniform(jitter_key, (CONV_CH,), jnp.float32, -0.3, 0.3)
    column_scale = 10.0 ** channel_ramp * jnp.exp(jitter) / math.sqrt(KERNEL)
    return normal_part * column_scale[None, :]


def draw_conv_bias(key, part):
    jitter_key = jax.random.fold_in(key, 21)
    channel_ramp = jnp.arange(CONV_CH, dtype=jnp.float32) / CONV_CH
    jitter = jax.random.uniform(jitter_key, (CONV_CH,), jnp.float32, 0.5, 1.5)
    return (0.5 + 9.5 * channel_ramp) * jitter


def levels(rng, dims, split, low, largest):
    def one(dim, blocks):
        steps = jax.random.uniform(jax.random.fold_in(jax.random.fold_in(rng, 6), dim), (blocks,), jnp.float32, low / len(split), largest / len(split))
        return jnp.repeat(jnp.exp(steps), dims[dim] // blocks).reshape((-1,) + (1,) * (len(dims) - dim - 1))

    factor_of = one(*split[0])
    for cut in split[1:]:
        factor_of = factor_of * one(*cut)
    return factor_of


def gaussian(key, extent, scale, limit, split=(), held_as=jnp.bfloat16):
    gain = levels(key, extent, split, -0.22, 0.18) if split else 1.0
    drawn = jax.random.normal(key, extent, jnp.float32) * scale * gain
    return jnp.minimum(jnp.maximum(drawn, -limit), limit).astype(held_as)


def setup_inputs(seed: int = 0) -> dict:
    key_of = jax.random.split(jax.random.key(seed), 14)
    tokens = gaussian(key_of[0], (TOKENS, D), 1.0, 6.0, ((0, 8),))
    norm_gain = jnp.clip(1.0 + 0.18 * jax.random.normal(key_of[1], (D,), jnp.float32), 0.1, 1.9)
    w_query = draw_w_query(jax.random.fold_in(key_of[13], 71), 0)
    w_key = gaussian(key_of[3], (D, KV_HEADS * HEAD_DIM), D ** -0.5, 0.125, ((0, 8), (1, 4)))
    w_value = gaussian(key_of[4], (D, KV_HEADS * HEAD_DIM), D ** -0.5, 0.125, ((0, 8), (1, 4)))
    w_content = gaussian(key_of[5], (D, CONV_CH), D ** -0.5, 0.125, ((0, 8), (1, 4)))
    w_gate = gaussian(key_of[6], (D, CONV_CH), D ** -0.5, 0.125, ((0, 8), (1, 4)))
    sink_logit = jnp.clip(1.0 + 5.0 * jax.random.uniform(key_of[7], (HEADS,), jnp.float32) ** levels(key_of[7], (HEADS,), ((0, 4),), -0.2, 0.2), 1.0, 6.0)
    conv_weight = draw_conv_weight(jax.random.fold_in(key_of[13], 71), 0)
    conv_bias = draw_conv_bias(jax.random.fold_in(key_of[13], 71), 0)
    channel_gain = jnp.clip(1.0 + 0.18 * jax.random.normal(key_of[10], (CONV_CH,), jnp.float32), 0.1, 1.9)
    out_attn = gaussian(key_of[11], (ATTN_W, D), (ATTN_W // 16) ** -0.5, 0.75, ((0, 4), (1, 8)))
    out_conv = gaussian(key_of[12], (CONV_CH, D), CONV_CH ** -0.5, 0.1875, ((0, 4), (1, 8)))
    return {"tokens": tokens, "norm_gain": norm_gain, "w_query": w_query, "w_key": w_key, "w_value": w_value, "w_content": w_content, "w_gate": w_gate, "sink_logit": sink_logit, "conv_weight": conv_weight, "conv_bias": conv_bias, "channel_gain": channel_gain, "out_attn": out_attn, "out_conv": out_conv}


EPS = 1e-05
THETA = 10000.0

def rotate(heads_in, positions):
    half_dim = heads_in.shape[-1] // 2
    inverse = 1.0 / THETA ** (jnp.arange(half_dim, dtype=jnp.float32) * 2.0 / heads_in.shape[-1])
    angles = positions.astype(jnp.float32)[:, None] * inverse[None, :]
    cosine = jnp.cos(angles)[:, None, :]
    sine_part = jnp.sin(angles)[:, None, :]
    former = heads_in[..., :half_dim]
    latter = heads_in[..., half_dim:]
    return jnp.concatenate([former * cosine - latter * sine_part, latter * cosine + former * sine_part], axis=-1)

def reference(tokens, norm_gain, w_query, w_key, w_value, w_content, w_gate, sink_logit, conv_weight, conv_bias, channel_gain, out_attn, out_conv):
    token_count = tokens.shape[0]
    positions = jnp.arange(token_count, dtype=jnp.int32)
    tokens_wide = tokens.astype(jnp.float32)
    inv_rms = lax.rsqrt(lax.optimization_barrier(jnp.mean(tokens_wide * tokens_wide, axis=1, keepdims=True)) + EPS)
    scaled = (tokens_wide * norm_gain[None, :]).astype(jnp.bfloat16)

    def project(weight):
        return jnp.dot(scaled, weight, preferred_element_type=jnp.float32) * inv_rms
    queries = rotate(project(w_query).reshape(token_count, HEADS, HEAD_DIM), positions).astype(jnp.bfloat16)
    key_rows = rotate(project(w_key).reshape(token_count, KV_HEADS, HEAD_DIM), positions).astype(jnp.bfloat16)
    value_rows = project(w_value).astype(jnp.bfloat16).reshape(token_count, KV_HEADS, HEAD_DIM)
    glu_out = (project(w_content) * jax.nn.sigmoid(project(w_gate))).astype(jnp.bfloat16)
    group_size = HEADS // KV_HEADS
    block_rows = math.gcd(token_count, 512)
    key_pad = jnp.concatenate([jnp.zeros((WINDOW, KV_HEADS, HEAD_DIM), jnp.bfloat16), key_rows], 0)
    value_pad = jnp.concatenate([jnp.zeros((WINDOW, KV_HEADS, HEAD_DIM), jnp.bfloat16), value_rows], 0)
    sink_col = sink_logit.reshape(KV_HEADS, group_size)[:, :, None, None]

    def attend(block_start):
        query_blk = lax.dynamic_slice_in_dim(queries, block_start, block_rows, 0).astype(jnp.float32)
        query_blk = query_blk.reshape(block_rows, KV_HEADS, group_size, HEAD_DIM)
        key_blk = lax.dynamic_slice_in_dim(key_pad, block_start, block_rows + WINDOW, 0).astype(jnp.float32)
        value_blk = lax.dynamic_slice_in_dim(value_pad, block_start, block_rows + WINDOW, 0).astype(jnp.float32)
        scores = jnp.einsum('qkgd,jkd->kgqj', query_blk, key_blk) * HEAD_DIM ** (-0.5)
        query_pos = block_start + jnp.arange(block_rows, dtype=jnp.int32)
        key_pos = block_start - WINDOW + jnp.arange(block_rows + WINDOW, dtype=jnp.int32)
        distance = query_pos[:, None] - key_pos[None, :]
        allowed = (distance >= 0) & (distance < WINDOW) & (key_pos[None, :] >= 0)
        scores = jnp.where(allowed[None, None], scores, -1e+30)
        row_max = jnp.maximum(lax.optimization_barrier(jnp.max(scores, axis=-1, keepdims=True)), sink_col)
        weights = jnp.exp(scores - row_max)
        denominator = lax.optimization_barrier(jnp.sum(weights, axis=-1, keepdims=True)) + jnp.exp(sink_col - row_max)
        probability = (weights / denominator).astype(jnp.bfloat16)
        attended = jnp.einsum('kgqj,jkd->qkgd', probability.astype(jnp.float32), value_blk)
        return attended.reshape(block_rows, HEADS * HEAD_DIM).astype(jnp.bfloat16)
    starts = jnp.arange(0, token_count, block_rows, dtype=jnp.int32)
    attn_out = lax.map(attend, starts).reshape(token_count, HEADS * HEAD_DIM)
    padded = jnp.concatenate([jnp.zeros((KERNEL - 1, CONV_CH), jnp.bfloat16), glu_out], 0)
    conv_sum = jnp.zeros((token_count, CONV_CH), jnp.float32) + conv_bias[None, :]
    for tap_index in range(KERNEL):
        window_rows = lax.slice_in_dim(padded, tap_index, tap_index + token_count, axis=0)
        conv_sum = conv_sum + conv_weight[tap_index][None, :] * window_rows.astype(jnp.float32)
    centre = lax.optimization_barrier(jnp.mean(conv_sum, axis=1, keepdims=True))
    centred = conv_sum - centre
    variance = lax.optimization_barrier(jnp.mean(centred * centred, axis=1, keepdims=True))
    conv_out = jax.nn.silu(centred * lax.rsqrt(variance + EPS) * channel_gain[None, :]).astype(jnp.bfloat16)
    attn_share = HEADS * HEAD_DIM // N_TP
    conv_share = CONV_CH // N_TP
    result = jnp.zeros((token_count, D), jnp.float32)
    for member in range(N_TP):
        partial_sum = jnp.dot(attn_out[:, member * attn_share:(member + 1) * attn_share], out_attn[member * attn_share:(member + 1) * attn_share], preferred_element_type=jnp.float32)
        partial_sum = partial_sum + jnp.dot(conv_out[:, member * conv_share:(member + 1) * conv_share], out_conv[member * conv_share:(member + 1) * conv_share], preferred_element_type=jnp.float32)
        rounded = lax.optimization_barrier(partial_sum.astype(jnp.bfloat16))
        result = result + rounded.astype(jnp.float32)
    return result.astype(jnp.bfloat16)
```

```python
import functools
import math

import jax
import jax.numpy as jnp
from jax import lax
from jax.experimental import pallas as pl
from jax.experimental.pallas import tpu as pltpu
from jax.sharding import PartitionSpec as P

HEAD_DIM = 64
CONV_CH = 1024
KERNEL = 31
WINDOW = 128


EPS = 1e-05
THETA = 10000.0


def shifted(block, axis, distance):
    devices = range(lax.axis_size(axis))
    route = [(i - distance, i) for i in devices if i - distance in devices]
    return lax.ppermute(block, axis, route)


def rotate(heads_in, positions):
    half_dim = heads_in.shape[-1] // 2
    inverse = 1.0 / THETA ** (jnp.arange(half_dim, dtype=jnp.float32) * 2.0 / heads_in.shape[-1])
    angles = positions.astype(jnp.float32)[:, None] * inverse[None, :]
    cosine = jnp.cos(angles)[:, None, :]
    sine_part = jnp.sin(angles)[:, None, :]
    former = heads_in[..., :half_dim]
    latter = heads_in[..., half_dim:]
    return jnp.concatenate(
        [former * cosine - latter * sine_part, latter * cosine + former * sine_part], axis=-1
    )


MESH = pl.DeviceIdType.MESH
LANES = 128
VMEM_GRANT = 60 * 1024 * 1024


def ring_place(index, n):
    odd = index % 2
    return (index // 2) * (1 - odd) + (n - 1 - index // 2) * odd


def ring_member(place, n):
    return jnp.where(place < (n + 1) // 2, 2 * place, 2 * (n - 1 - place) + 1)


def greet(peers):
    barrier = pltpu.get_barrier_semaphore()
    for peer in peers:
        pl.semaphore_signal(barrier, inc=1, device_id=peer, device_id_type=MESH)
    pl.semaphore_wait(barrier, len(peers))


def project_kernel(
    n, pieces, tok_ref, gain_ref, w_ref, o_ref, proj_ref, og_ref,
    scaled, inv, wg, w_send, w_recv, o_send, o_recv,
):
    me = lax.axis_index("sp")
    place = ring_place(me, n)
    after = {"sp": ring_member(lax.rem(place + 1, n), n)}
    before = {"sp": ring_member(lax.rem(place + n - 1, n), n)}
    greet((after, before))

    def hop(own, held, send, recv, d, c, s):
        half = own.shape[0] // 2
        sub = half // pieces
        rows = pl.ds(d * half + c * sub, sub)
        offset = n - s if d == 0 else s
        owner = ring_member(lax.rem(place + offset, n), n)
        return pltpu.make_async_remote_copy(
            src_ref=own.at[rows] if s == 0 else held.at[owner, rows],
            dst_ref=held.at[owner, rows],
            send_sem=send.at[d, s, c],
            recv_sem=recv.at[d, s, c],
            device_id=after if d == 0 else before,
            device_id_type=MESH,
        )

    def w_hop(d, c, s):
        return hop(w_ref, wg, w_send, w_recv, d, c, s)

    def o_hop(d, c, s):
        return hop(o_ref, og_ref, o_send, o_recv, d, c, s)

    lanes = [(d, c) for c in range(pieces) for d in range(2)]
    for d, c in lanes:
        w_hop(d, c, 0).start()
    for d, c in lanes:
        o_hop(d, c, 0).start()

    token_count, width = tok_ref.shape
    depth = w_ref.shape[0]
    step_rows = math.gcd(token_count, 64)

    @pl.loop(0, token_count // step_rows)
    def _(i):
        rows = pl.ds(pl.multiple_of(i * step_rows, step_rows), step_rows)
        wide = tok_ref[rows, :].astype(jnp.float32)
        inv[rows, :] = lax.rsqrt(jnp.sum(wide * wide, axis=1, keepdims=True) / width + EPS)
        scaled[rows, :] = (wide * gain_ref[...]).astype(jnp.bfloat16)

    tile = math.gcd(token_count, 256)
    og_ref[me] = o_ref[...]

    def add(terms, first, last):
        @pl.loop(0, token_count // tile)
        def _(i):
            rows = pl.ds(pl.multiple_of(i * tile, tile), tile)
            total = None if first else proj_ref[rows, :]
            for owner, block in terms:
                columns = pl.ds(pl.multiple_of(owner * depth, depth), depth)
                term = jnp.dot(
                    scaled[rows, columns], block(), preferred_element_type=jnp.float32
                )
                total = term if total is None else total + term
            proj_ref[rows, :] = total * inv[rows, :] if last else total

    add([(me, lambda: w_ref[...])], True, n == 1)
    for t in range(n - 1):
        for d, c in lanes:
            w_hop(d, c, t).wait_recv()
            if t < n - 2:
                w_hop(d, c, t + 1).start()
        for d, c in lanes:
            o_hop(d, c, t).wait_recv()
            if t < n - 2:
                o_hop(d, c, t + 1).start()
        ready = [k for k in range(1, n) if max(k, n - k) - 1 == t]
        if ready:
            owners = [ring_member(lax.rem(place + n - k, n), n) for k in ready]
            add([(o, lambda o=o: wg[o]) for o in owners], False, t == n - 2)
    for t in range(n - 1):
        for d, c in lanes:
            w_hop(d, c, t).wait_send()
            o_hop(d, c, t).wait_send()


def gather_and_project(n, tokens, gain, w_own, o_own):
    token_count = tokens.shape[0]
    width = w_own.shape[1]
    pieces = 2
    sems = pltpu.SemaphoreType.DMA((2, n - 1, pieces))
    vmem = pl.BlockSpec(memory_space=pltpu.VMEM)
    return pl.pallas_call(
        functools.partial(project_kernel, n, pieces),
        out_shape=(
            jax.ShapeDtypeStruct((token_count, width), jnp.float32),
            jax.ShapeDtypeStruct((n,) + o_own.shape, jnp.bfloat16),
        ),
        in_specs=[vmem] * 4,
        out_specs=(vmem, vmem),
        scratch_shapes=[
            pltpu.VMEM(tokens.shape, jnp.bfloat16),
            pltpu.VMEM((token_count, 1), jnp.float32),
            pltpu.VMEM((n,) + w_own.shape, jnp.bfloat16),
            sems, sems, sems, sems,
        ],
        compiler_params=pltpu.CompilerParams(
            collective_id=0, has_side_effects=True, vmem_limit_bytes=VMEM_GRANT
        ),
        name="gather_project",
    )(tokens, gain[None, :], w_own, o_own)


def mix_kernel(
    parts, act_ref, og_ref, out_ref, near_out, near_in, far_out, far_in,
    near_send, near_recv, far_send, far_recv,
):
    me = lax.axis_index("tp")
    core = me % 2
    near = me + 1 - 2 * core
    far = lax.rem(me + 2, 4)
    far_near = lax.rem(near + 2, 4)
    near_id, far_id = {"tp": near}, {"tp": far}
    greet((near_id, far_id))
    rows_out = out_ref.shape[0]
    blocks = og_ref.shape[0] // parts
    cols = og_ref.shape[2]

    def partial_of(member, q):
        rows = pl.ds(pl.multiple_of(member * rows_out, rows_out), rows_out)
        acts = act_ref[rows, :]
        return jnp.concatenate(
            [
                jnp.dot(acts, og_ref[q * blocks + b], preferred_element_type=jnp.float32)
                for b in range(blocks)
            ],
            axis=1,
        )

    def near_copy(which, q):
        return pltpu.make_async_remote_copy(
            src_ref=near_out.at[which, q],
            dst_ref=near_in.at[which, q],
            send_sem=near_send.at[which, q],
            recv_sem=near_recv.at[which, q],
            device_id=near_id,
            device_id_type=MESH,
        )

    def far_copy(q):
        return pltpu.make_async_remote_copy(
            src_ref=far_out.at[q],
            dst_ref=far_in.at[q],
            send_sem=far_send.at[q],
            recv_sem=far_recv.at[q],
            device_id=far_id,
            device_id_type=MESH,
        )

    def give_near(which, member, q):
        near_out[which, q] = partial_of(member, q).astype(jnp.bfloat16)
        near_copy(which, q).start()

    def give_far(q):
        mine = partial_of(far, q)
        near_copy(0, q).wait_recv()
        far_out[q] = (mine + near_in[0, q].astype(jnp.float32)).astype(jnp.bfloat16)
        far_copy(q).start()

    give_near(0, far_near, 0)
    for q in range(1, parts):
        give_near(0, far_near, q)
        give_far(q - 1)
    give_far(parts - 1)
    for q in range(parts):
        give_near(1, near, q)
    for q in range(parts):
        mine = partial_of(me, q)
        near_copy(1, q).wait_recv()
        mine = mine + near_in[1, q].astype(jnp.float32)
        far_copy(q).wait_recv()
        span = blocks * cols
        out_ref[:, q * span : (q + 1) * span] = (
            mine + far_in[q].astype(jnp.float32)
        ).astype(jnp.bfloat16)
    for q in range(parts):
        near_copy(0, q).wait_send()
        near_copy(1, q).wait_send()
        far_copy(q).wait_send()


def mix_and_scatter(acts, og):
    n, _, cols = og.shape
    parts = math.gcd(n, 4)
    rows_out = acts.shape[0] // 4
    span = n // parts * cols
    vmem = pl.BlockSpec(memory_space=pltpu.VMEM)
    return pl.pallas_call(
        functools.partial(mix_kernel, parts),
        out_shape=jax.ShapeDtypeStruct((rows_out, n * cols), jnp.bfloat16),
        in_specs=[vmem] * 2,
        out_specs=vmem,
        scratch_shapes=[
            pltpu.VMEM((2, parts, rows_out, span), jnp.bfloat16),
            pltpu.VMEM((2, parts, rows_out, span), jnp.bfloat16),
            pltpu.VMEM((parts, rows_out, span), jnp.bfloat16),
            pltpu.VMEM((parts, rows_out, span), jnp.bfloat16),
            pltpu.SemaphoreType.DMA((2, parts)),
            pltpu.SemaphoreType.DMA((2, parts)),
            pltpu.SemaphoreType.DMA((parts,)),
            pltpu.SemaphoreType.DMA((parts,)),
        ],
        compiler_params=pltpu.CompilerParams(
            collective_id=1, has_side_effects=True, vmem_limit_bytes=VMEM_GRANT
        ),
        name="mix_scatter",
    )(acts, og)


def plain_shards(
    tokens,
    norm_gain,
    w_query,
    w_key,
    w_value,
    w_content,
    w_gate,
    sink_logit,
    conv_weight,
    conv_bias,
    channel_gain,
    out_attn,
    out_conv,
):
    token_count = tokens.shape[0]
    offset = lax.axis_index("sp") * token_count
    positions = offset + jnp.arange(token_count, dtype=jnp.int32)
    tokens_wide = tokens.astype(jnp.float32)
    inv_rms = lax.rsqrt(jnp.mean(tokens_wide * tokens_wide, axis=1, keepdims=True) + EPS)
    scaled = (tokens_wide * norm_gain[None, :]).astype(jnp.bfloat16)
    widths = [
        w_query.shape[1],
        w_key.shape[1],
        w_value.shape[1],
        w_content.shape[1],
        w_gate.shape[1],
    ]
    whole_weights = (
        lax.all_gather(w_query, "sp", axis=0, tiled=True),
        lax.all_gather(w_key, "sp", axis=0, tiled=True),
        lax.all_gather(w_value, "sp", axis=0, tiled=True),
        lax.all_gather(w_content, "sp", axis=0, tiled=True),
        lax.all_gather(w_gate, "sp", axis=0, tiled=True),
    )
    joined_whole = jnp.concatenate(whole_weights, axis=1)
    projected = jnp.dot(scaled, joined_whole, preferred_element_type=jnp.float32)
    projected = projected * inv_rms
    bounds = [0]
    for width in widths:
        bounds.append(bounds[-1] + width)
    proj_query = projected[:, bounds[0] : bounds[1]]
    proj_key = projected[:, bounds[1] : bounds[2]]
    proj_value = projected[:, bounds[2] : bounds[3]]
    proj_content = projected[:, bounds[3] : bounds[4]]
    proj_gate = projected[:, bounds[4] : bounds[5]]
    kv_local = widths[1] // HEAD_DIM
    heads_local = widths[0] // HEAD_DIM
    group_size = heads_local // kv_local
    queries = rotate(proj_query.reshape(token_count, heads_local, HEAD_DIM), positions).astype(
        jnp.bfloat16
    )
    key_rows = rotate(proj_key.reshape(token_count, kv_local, HEAD_DIM), positions).astype(
        jnp.bfloat16
    )
    value_rows = proj_value.astype(jnp.bfloat16).reshape(token_count, kv_local, HEAD_DIM)
    glu_out = (proj_content * jax.nn.sigmoid(proj_gate)).astype(jnp.bfloat16)
    prior_key, prior_value, prior_glu = shifted(
        (
            key_rows[token_count - WINDOW :],
            value_rows[token_count - WINDOW :],
            glu_out[token_count - (KERNEL - 1) :],
        ),
        "sp",
        1,
    )
    key_ext = jnp.concatenate([prior_key, key_rows], 0)
    value_ext = jnp.concatenate([prior_value, value_rows], 0)
    block_rows = math.gcd(token_count, 512)
    sink_col = sink_logit.reshape(kv_local, group_size)[:, :, None, None]

    def attend(block_start):
        query_blk = lax.dynamic_slice_in_dim(queries, block_start, block_rows, 0).reshape(
            block_rows, kv_local, group_size, HEAD_DIM
        )
        key_blk = lax.dynamic_slice_in_dim(key_ext, block_start, block_rows + WINDOW, 0)
        value_blk = lax.dynamic_slice_in_dim(value_ext, block_start, block_rows + WINDOW, 0)
        scores = jnp.einsum(
            "qkgd,jkd->kgqj", query_blk, key_blk, preferred_element_type=jnp.float32
        ) * HEAD_DIM ** (-0.5)
        query_pos = offset + block_start + jnp.arange(block_rows, dtype=jnp.int32)
        key_pos = offset + block_start - WINDOW + jnp.arange(block_rows + WINDOW, dtype=jnp.int32)
        distance = query_pos[:, None] - key_pos[None, :]
        allowed = (distance >= 0) & (distance < WINDOW) & (key_pos[None, :] >= 0)
        scores = jnp.where(allowed[None, None], scores, -1e30)
        row_max = jnp.maximum(jnp.max(scores, axis=-1, keepdims=True), sink_col)
        weights = jnp.exp(scores - row_max)
        denominator = jnp.sum(weights, axis=-1, keepdims=True) + jnp.exp(sink_col - row_max)
        probability = (weights / denominator).astype(jnp.bfloat16)
        attended = jnp.einsum(
            "kgqj,jkd->qkgd", probability, value_blk, preferred_element_type=jnp.float32
        )
        return attended.reshape(block_rows, heads_local * HEAD_DIM).astype(jnp.bfloat16)

    starts = jnp.arange(0, token_count, block_rows, dtype=jnp.int32)
    attn_out = lax.map(attend, starts).reshape(token_count, heads_local * HEAD_DIM)
    padded = jnp.concatenate([prior_glu, glu_out], 0)
    conv_sum = jnp.zeros(glu_out.shape, jnp.float32) + conv_bias[None, :]
    for tap_index in range(KERNEL):
        window_rows = lax.slice_in_dim(padded, tap_index, tap_index + token_count, axis=0)
        conv_sum = conv_sum + conv_weight[tap_index][None, :] * window_rows.astype(jnp.float32)
    row_sum, row_squares = lax.psum(
        (jnp.sum(conv_sum, axis=1), jnp.sum(conv_sum * conv_sum, axis=1)), "tp"
    )
    centre = row_sum / CONV_CH
    variance = jnp.maximum(row_squares / CONV_CH - centre * centre, 0.0)
    centred = conv_sum - centre[:, None]
    conv_out = jax.nn.silu(
        centred * lax.rsqrt(variance + EPS)[:, None] * channel_gain[None, :]
    ).astype(jnp.bfloat16)
    attn_weight, conv_weight_out = (
        lax.all_gather(out_attn, "sp", axis=1, tiled=True),
        lax.all_gather(out_conv, "sp", axis=1, tiled=True),
    )
    return lax.psum_scatter(
        (
            jnp.dot(attn_out, attn_weight, preferred_element_type=jnp.float32)
            + jnp.dot(conv_out, conv_weight_out, preferred_element_type=jnp.float32)
        ).astype(jnp.bfloat16),
        "tp",
        scatter_dimension=0,
        tiled=True,
    )


def ring_shards(
    tokens,
    norm_gain,
    w_query,
    w_key,
    w_value,
    w_content,
    w_gate,
    sink_logit,
    conv_weight,
    conv_bias,
    channel_gain,
    out_attn,
    out_conv,
):
    token_count = tokens.shape[0]
    offset = lax.axis_index("sp") * token_count
    positions = offset + jnp.arange(token_count, dtype=jnp.int32)
    widths = [
        w_query.shape[1],
        w_key.shape[1],
        w_value.shape[1],
        w_content.shape[1],
        w_gate.shape[1],
    ]
    w_own = jnp.concatenate([w_query, w_key, w_value, w_content, w_gate], axis=1)
    o_own = jnp.concatenate([out_attn, out_conv], axis=0)
    projected, mix_weight = gather_and_project(
        lax.axis_size("sp"), tokens, norm_gain, w_own, o_own
    )
    bounds = [0]
    for width in widths:
        bounds.append(bounds[-1] + width)
    proj_query = projected[:, bounds[0] : bounds[1]]
    proj_key = projected[:, bounds[1] : bounds[2]]
    proj_value = projected[:, bounds[2] : bounds[3]]
    proj_content = projected[:, bounds[3] : bounds[4]]
    proj_gate = projected[:, bounds[4] : bounds[5]]
    kv_local = widths[1] // HEAD_DIM
    heads_local = widths[0] // HEAD_DIM
    group_size = heads_local // kv_local
    queries = rotate(proj_query.reshape(token_count, heads_local, HEAD_DIM), positions).astype(
        jnp.bfloat16
    )
    key_rows = rotate(proj_key.reshape(token_count, kv_local, HEAD_DIM), positions).astype(
        jnp.bfloat16
    )
    value_rows = proj_value.astype(jnp.bfloat16).reshape(token_count, kv_local, HEAD_DIM)
    glu_out = (proj_content * jax.nn.sigmoid(proj_gate)).astype(jnp.bfloat16)
    prior_key, prior_value, prior_glu = shifted(
        (
            key_rows[token_count - WINDOW :],
            value_rows[token_count - WINDOW :],
            glu_out[token_count - (KERNEL - 1) :],
        ),
        "sp",
        1,
    )
    key_ext = jnp.concatenate([prior_key, key_rows], 0)
    value_ext = jnp.concatenate([prior_value, value_rows], 0)
    blocks = token_count // WINDOW
    sink_col = sink_logit.reshape(kv_local, group_size)[None, :, :, None, None]
    query_blk = queries.reshape(blocks, WINDOW, kv_local, group_size, HEAD_DIM)

    def windows(ext):
        cut = ext.reshape(blocks + 1, WINDOW, kv_local, HEAD_DIM)
        return jnp.concatenate([cut[:-1], cut[1:]], axis=1)

    scores = jnp.einsum(
        "bqkgd,bjkd->bkgqj", query_blk, windows(key_ext), preferred_element_type=jnp.float32
    ) * HEAD_DIM ** (-0.5)
    query_off = jnp.arange(WINDOW, dtype=jnp.int32)
    key_off = jnp.arange(2 * WINDOW, dtype=jnp.int32) - WINDOW
    distance = query_off[:, None] - key_off[None, :]
    key_pos = offset + jnp.arange(blocks, dtype=jnp.int32)[:, None] * WINDOW + key_off[None, :]
    allowed = ((distance >= 0) & (distance < WINDOW))[None] & (key_pos >= 0)[:, None, :]
    scores = jnp.where(allowed[:, None, None], scores, -1e30)
    row_max = jnp.maximum(jnp.max(scores, axis=-1, keepdims=True), sink_col)
    weights = jnp.exp(scores - row_max)
    denominator = jnp.sum(weights, axis=-1, keepdims=True) + jnp.exp(sink_col - row_max)
    probability = (weights / denominator).astype(jnp.bfloat16)
    attended = jnp.einsum(
        "bkgqj,bjkd->bqkgd", probability, windows(value_ext), preferred_element_type=jnp.float32
    )
    attn_out = attended.reshape(token_count, heads_local * HEAD_DIM).astype(jnp.bfloat16)
    padded = jnp.concatenate([prior_glu, glu_out], 0)
    conv_sum = jnp.zeros(glu_out.shape, jnp.float32) + conv_bias[None, :]
    for tap_index in range(KERNEL):
        window_rows = lax.slice_in_dim(padded, tap_index, tap_index + token_count, axis=0)
        conv_sum = conv_sum + conv_weight[tap_index][None, :] * window_rows.astype(jnp.float32)
    row_sum, row_squares = lax.psum(
        (jnp.sum(conv_sum, axis=1), jnp.sum(conv_sum * conv_sum, axis=1)), "tp"
    )
    centre = row_sum / CONV_CH
    variance = jnp.maximum(row_squares / CONV_CH - centre * centre, 0.0)
    centred = conv_sum - centre[:, None]
    conv_out = jax.nn.silu(
        centred * lax.rsqrt(variance + EPS)[:, None] * channel_gain[None, :]
    ).astype(jnp.bfloat16)
    return mix_and_scatter(jnp.concatenate([attn_out, conv_out], axis=1), mix_weight)


def solution(mesh):
    placed = (
        P("sp", None),
        P(),
        P("sp", "tp"),
        P("sp", "tp"),
        P("sp", "tp"),
        P("sp", "tp"),
        P("sp", "tp"),
        P("tp"),
        P(None, "tp"),
        P("tp"),
        P("tp"),
        P("tp", "sp"),
        P("tp", "sp"),
    )
    sp, tp = mesh.shape["sp"], mesh.shape["tp"]
    ringed = tp == 4 and sp % 2 == 0

    def shards(*arrays):
        fits = (
            ringed
            and arrays[11].shape[1] % LANES == 0
            and arrays[2].shape[0] % LANES == 0
            and arrays[0].shape[0] % (WINDOW * tp) == 0
        )
        return (ring_shards if fits else plain_shards)(*arrays)

    return jax.shard_map(
        shards, mesh=mesh, in_specs=placed, out_specs=P(("sp", "tp"), None), check_vma=False
    )
```

```python
import functools
import math

import jax
import jax.numpy as jnp
from jax import lax
from jax.experimental import pallas as pl
from jax.experimental.pallas import tpu as pltpu
from jax.sharding import PartitionSpec as P

HEAD_DIM = 64
CONV_CH = 1024
KERNEL = 31
WINDOW = 128


EPS = 1e-05
THETA = 10000.0


def shifted(block, axis, distance):
    devices = range(lax.axis_size(axis))
    route = [(i - distance, i) for i in devices if i - distance in devices]
    return lax.ppermute(block, axis, route)


def rotate(heads_in, positions):
    half_dim = heads_in.shape[-1] // 2
    inverse = 1.0 / THETA ** (jnp.arange(half_dim, dtype=jnp.float32) * 2.0 / heads_in.shape[-1])
    angles = positions.astype(jnp.float32)[:, None] * inverse[None, :]
    cosine = jnp.cos(angles)[:, None, :]
    sine_part = jnp.sin(angles)[:, None, :]
    former = heads_in[..., :half_dim]
    latter = heads_in[..., half_dim:]
    return jnp.concatenate(
        [former * cosine - latter * sine_part, latter * cosine + former * sine_part], axis=-1
    )


MESH = pl.DeviceIdType.MESH
LANES = 128
VMEM_GRANT = 60 * 1024 * 1024


def ring_place(index, n):
    odd = index % 2
    return (index // 2) * (1 - odd) + (n - 1 - index // 2) * odd


def ring_member(place, n):
    return jnp.where(place < (n + 1) // 2, 2 * place, 2 * (n - 1 - place) + 1)


def greet(peers):
    barrier = pltpu.get_barrier_semaphore()
    for peer in peers:
        pl.semaphore_signal(barrier, inc=1, device_id=peer, device_id_type=MESH)
    pl.semaphore_wait(barrier, len(peers))


def project_kernel(
    n, pieces, head_lanes,
    tok_ref, gain_ref, w_ref, o_ref, cos_ref, sin_ref, sink_ref, taps_ref, bias_ref, chan_ref,
    act_ref, og_ref,
    scaled, inv, wg, proj_ref, turned, key_ext, value_ext, glu_ext, conv, stats, peer_stats,
    w_send, w_recv, o_send, o_recv, halo_send, halo_recv, stat_send, stat_recv,
):
    me = lax.axis_index("sp")
    place = ring_place(me, n)
    after = {"sp": ring_member(lax.rem(place + 1, n), n)}
    before = {"sp": ring_member(lax.rem(place + n - 1, n), n)}
    following = {"sp": lax.rem(me + 1, n)}
    previous = {"sp": lax.rem(me + n - 1, n)}
    members = lax.axis_size("tp")
    mine_tp = lax.axis_index("tp")
    siblings = [{"tp": lax.rem(mine_tp + k, members)} for k in range(1, members)]
    greet([after, before, following, previous] + siblings)

    def hop(own, held, send, recv, d, c, s):
        half = own.shape[0] // 2
        sub = half // pieces
        rows = pl.ds(d * half + c * sub, sub)
        offset = n - s if d == 0 else s
        owner = ring_member(lax.rem(place + offset, n), n)
        return pltpu.make_async_remote_copy(
            src_ref=own.at[rows] if s == 0 else held.at[owner, rows],
            dst_ref=held.at[owner, rows],
            send_sem=send.at[d, s, c],
            recv_sem=recv.at[d, s, c],
            device_id=after if d == 0 else before,
            device_id_type=MESH,
        )

    def w_hop(d, c, s):
        return hop(w_ref, wg, w_send, w_recv, d, c, s)

    def o_hop(d, c, s):
        return hop(o_ref, og_ref, o_send, o_recv, d, c, s)

    lanes = [(d, c) for c in range(pieces) for d in range(2)]
    for d, c in lanes:
        w_hop(d, c, 0).start()

    token_count, width = tok_ref.shape
    depth = w_ref.shape[0]
    step_rows = math.gcd(token_count, 64)

    @pl.loop(0, token_count // step_rows)
    def _(i):
        rows = pl.ds(pl.multiple_of(i * step_rows, step_rows), step_rows)
        wide = tok_ref[rows, :].astype(jnp.float32)
        inv[rows, :] = lax.rsqrt(jnp.sum(wide * wide, axis=1, keepdims=True) / width + EPS)
        scaled[rows, :] = (wide * gain_ref[...]).astype(jnp.bfloat16)

    tile = math.gcd(token_count, 256)
    og_ref[me] = o_ref[...]

    def add(terms, first, last):
        @pl.loop(0, token_count // tile)
        def _(i):
            rows = pl.ds(pl.multiple_of(i * tile, tile), tile)
            total = None if first else proj_ref[rows, :]
            for owner, block in terms:
                columns = pl.ds(pl.multiple_of(owner * depth, depth), depth)
                term = jnp.dot(
                    scaled[rows, columns], block(), preferred_element_type=jnp.float32
                )
                total = term if total is None else total + term
            proj_ref[rows, :] = total * inv[rows, :] if last else total

    add([(me, lambda: w_ref[...])], True, n == 1)
    for t in range(n - 1):
        for d, c in lanes:
            w_hop(d, c, t).wait_recv()
            if t < n - 2:
                w_hop(d, c, t + 1).start()
        if t == max(n - 3, 0):
            for d, c in lanes:
                o_hop(d, c, 0).start()
        ready = [k for k in range(1, n) if max(k, n - k) - 1 == t]
        if ready:
            owners = [ring_member(lax.rem(place + n - k, n), n) for k in ready]
            add([(o, lambda o=o: wg[o]) for o in owners], False, t == n - 2)

    def o_advance(t):
        if t >= n - 1:
            return
        for d, c in lanes:
            o_hop(d, c, t).wait_recv()
            if t < n - 2:
                o_hop(d, c, t + 1).start()

    head_w = LANES // 2
    channels = taps_ref.shape[1]
    at_glu = head_lanes + LANES
    lead = glu_ext.shape[0] - token_count
    tiles = token_count // WINDOW

    def lane_of(shape):
        return lax.broadcasted_iota(jnp.int32, shape, 1)

    def turn(x, cosine, sine_part):
        low = lane_of(x.shape) % head_w < head_w // 2
        swapped = jnp.where(
            low, pltpu.roll(x, LANES - head_w // 2, 1), pltpu.roll(x, head_w // 2, 1)
        )
        return x * cosine + swapped * sine_part

    def shape_rows(i):
        base = pl.multiple_of(i * WINDOW, WINDOW)
        rows = pl.ds(base, WINDOW)
        cosine, sine_part = cos_ref[rows, :], sin_ref[rows, :]
        for start in range(0, head_lanes, LANES):
            cut = slice(start, start + LANES)
            turned[rows, cut] = turn(proj_ref[rows, cut], cosine, sine_part).astype(jnp.bfloat16)
        pair = proj_ref[rows, head_lanes:at_glu]
        key_part = turn(pair, cosine, sine_part)
        low = lane_of(pair.shape) < head_w
        ext = pl.ds(base + WINDOW, WINDOW)
        key_ext[ext, :] = jnp.where(low, key_part, pltpu.roll(key_part, head_w, 1)).astype(
            jnp.bfloat16
        )
        value_ext[ext, :] = jnp.where(low, pltpu.roll(pair, head_w, 1), pair).astype(jnp.bfloat16)
        content = proj_ref[rows, at_glu : at_glu + channels]
        gate = proj_ref[rows, at_glu + channels : at_glu + 2 * channels]
        glu_ext[pl.ds(base + lead, WINDOW), :] = (
            (content * jax.nn.sigmoid(gate)).astype(jnp.bfloat16).astype(jnp.float32)
        )

    pl.loop(0, tiles)(shape_rows)

    def halo(which):
        ref, count = ((key_ext, WINDOW), (value_ext, WINDOW), (glu_ext, lead))[which]
        return pltpu.make_async_remote_copy(
            src_ref=ref.at[pl.ds(token_count, count)],
            dst_ref=ref.at[pl.ds(0, count)],
            send_sem=halo_send.at[which],
            recv_sem=halo_recv.at[which],
            device_id=following,
            device_id_type=MESH,
        )

    for which in range(3):
        halo(which).start()

    def convolve(i):
        base = pl.multiple_of(i * WINDOW, WINDOW)
        shift = lead - (KERNEL - 1)
        row_sum = row_squares = None
        for start in range(0, channels, LANES):
            cut = slice(start, start + LANES)
            parts = []
            for sub in range(0, WINDOW, 64):
                slab = glu_ext[pl.ds(base + sub, 64 + lead), cut]
                total = jnp.zeros((64, LANES), jnp.float32) + bias_ref[:, cut]
                for r in range(8):
                    moved = slab if r == 0 else pltpu.roll(slab, 64 + lead - r, 0)
                    for m in range(0, lead + 1, 8):
                        tap = m + r - shift
                        if 0 <= tap < KERNEL:
                            total = total + taps_ref[tap : tap + 1, cut] * moved[m : m + 64]
                parts.append(total)
            summed = jnp.concatenate(parts, axis=0)
            conv[pl.ds(base, WINDOW), cut] = summed
            one = jnp.sum(summed, axis=1, keepdims=True)
            two = jnp.sum(summed * summed, axis=1, keepdims=True)
            row_sum = one if row_sum is None else row_sum + one
            row_squares = two if row_squares is None else row_squares + two
        lane = lane_of((WINDOW, LANES))
        packed = jnp.where(lane == 0, row_sum, jnp.where(lane == 1, row_squares, 0.0))
        stats[:, pl.ds(base, WINDOW)] = packed.T[:8, :]

    half_tiles = max(tiles // 2, 1)
    pl.loop(1, half_tiles)(convolve)
    o_advance(0)
    pl.loop(half_tiles, tiles)(convolve)
    halo(2).wait_recv()
    glu_ext[0:lead, :] = jnp.where(me > 0, glu_ext[0:lead, :], 0.0)
    convolve(0)

    def stat_copy(k):
        return pltpu.make_async_remote_copy(
            src_ref=stats,
            dst_ref=peer_stats.at[k],
            send_sem=stat_send.at[k],
            recv_sem=stat_recv.at[k],
            device_id=siblings[k],
            device_id_type=MESH,
        )

    for k in range(members - 1):
        stat_copy(k).start()
    o_advance(1)

    def attend(i):
        base = pl.multiple_of(i * WINDOW, WINDOW)
        rows, reach = pl.ds(base, WINDOW), pl.ds(base, 2 * WINDOW)
        keys, values = key_ext[reach, :], value_ext[reach, :]
        shape = (WINDOW, 2 * WINDOW)
        column = lane_of(shape)
        distance = lax.broadcasted_iota(jnp.int32, shape, 0) - column + WINDOW
        first = me * token_count + i * WINDOW - WINDOW
        allowed = (distance >= 0) & (distance < WINDOW) & (column + first >= 0)
        low = lane_of((WINDOW, LANES)) < head_w
        for start in range(0, head_lanes, LANES):
            cut = slice(start, start + LANES)
            both = turned[rows, cut].astype(jnp.float32)
            found = []
            for side in range(2):
                sink = sink_ref[start // head_w + side]
                query = jnp.where(low if side == 0 else ~low, both, 0.0).astype(jnp.bfloat16)
                scores = lax.dot_general(
                    query, keys, (((1,), (1,)), ((), ())), preferred_element_type=jnp.float32
                ) * HEAD_DIM ** (-0.5)
                scores = jnp.where(allowed, scores, -1e30)
                row_max = jnp.maximum(jnp.max(scores, axis=1, keepdims=True), sink)
                weights = jnp.exp(scores - row_max)
                denominator = jnp.sum(weights, axis=1, keepdims=True) + jnp.exp(sink - row_max)
                probability = (weights * (1.0 / denominator)).astype(jnp.bfloat16)
                found.append(jnp.dot(probability, values, preferred_element_type=jnp.float32))
            act_ref[rows, cut] = jnp.where(low, found[0], found[1]).astype(jnp.bfloat16)

    pl.loop(1, half_tiles)(attend)
    o_advance(2)
    pl.loop(half_tiles, tiles)(attend)
    halo(0).wait_recv()
    halo(1).wait_recv()
    attend(0)
    o_advance(3)
    for k in range(members - 1):
        stat_copy(k).wait_recv()

    def normalise(i):
        base = pl.multiple_of(i * WINDOW, WINDOW)
        rows = pl.ds(base, WINDOW)
        total = stats[:, rows]
        for k in range(members - 1):
            total = total + peer_stats[k, :, rows]
        total = total * (1.0 / (channels * members))
        column = jnp.concatenate([total] * (LANES // 8), axis=0).T
        centre = column[:, 0:1]
        variance = jnp.maximum(column[:, 1:2] - centre * centre, 0.0)
        normed = (conv[rows, :] - centre) * lax.rsqrt(variance + EPS) * chan_ref[...]
        act_ref[rows, head_lanes : head_lanes + channels] = (
            normed * jax.nn.sigmoid(normed)
        ).astype(jnp.bfloat16)

    pl.loop(0, tiles)(normalise)
    for t in range(4, n - 1):
        o_advance(t)
    for which in range(3):
        halo(which).wait_send()
    for k in range(members - 1):
        stat_copy(k).wait_send()
    for t in range(n - 1):
        for d, c in lanes:
            w_hop(d, c, t).wait_send()
            o_hop(d, c, t).wait_send()


def gather_and_mix(n, tokens, gain, w_own, o_own, cosine, sine_part, sink, taps, bias, chan):
    token_count = tokens.shape[0]
    channels = taps.shape[1]
    head_lanes = sink.shape[0] * HEAD_DIM
    lead = -(-(KERNEL - 1) // 8) * 8
    members = lax.axis_size("tp")
    pieces = 2
    dma = pltpu.SemaphoreType.DMA
    sems = dma((2, n - 1, pieces))
    vmem = pl.BlockSpec(memory_space=pltpu.VMEM)
    smem = pl.BlockSpec(memory_space=pltpu.SMEM)
    return pl.pallas_call(
        functools.partial(project_kernel, n, pieces, head_lanes),
        out_shape=(
            jax.ShapeDtypeStruct((token_count, head_lanes + channels), jnp.bfloat16),
            jax.ShapeDtypeStruct((n,) + o_own.shape, jnp.bfloat16),
        ),
        in_specs=[vmem] * 6 + [smem] + [vmem] * 3,
        out_specs=(vmem, vmem),
        scratch_shapes=[
            pltpu.VMEM(tokens.shape, jnp.bfloat16),
            pltpu.VMEM((token_count, 1), jnp.float32),
            pltpu.VMEM((n,) + w_own.shape, jnp.bfloat16),
            pltpu.VMEM((token_count, w_own.shape[1]), jnp.float32),
            pltpu.VMEM((token_count, head_lanes), jnp.bfloat16),
            pltpu.VMEM((token_count + WINDOW, LANES), jnp.bfloat16),
            pltpu.VMEM((token_count + WINDOW, LANES), jnp.bfloat16),
            pltpu.VMEM((token_count + lead, channels), jnp.float32),
            pltpu.VMEM((token_count, channels), jnp.float32),
            pltpu.VMEM((8, token_count), jnp.float32),
            pltpu.VMEM((members - 1, 8, token_count), jnp.float32),
            sems, sems, sems, sems,
            dma((3,)), dma((3,)), dma((members - 1,)), dma((members - 1,)),
        ],
        compiler_params=pltpu.CompilerParams(
            collective_id=0, has_side_effects=True, vmem_limit_bytes=VMEM_GRANT
        ),
        name="gather_mix",
    )(
        tokens, gain[None, :], w_own, o_own, cosine, sine_part, sink, taps,
        bias[None, :], chan[None, :],
    )


def mix_kernel(
    parts, act_ref, og_ref, out_ref, near_out, near_in, far_out, far_in,
    near_send, near_recv, far_send, far_recv,
):
    me = lax.axis_index("tp")
    core = me % 2
    near = me + 1 - 2 * core
    far = lax.rem(me + 2, 4)
    far_near = lax.rem(near + 2, 4)
    near_id, far_id = {"tp": near}, {"tp": far}
    greet((near_id, far_id))
    rows_out = out_ref.shape[0]
    blocks = og_ref.shape[0] // parts
    cols = og_ref.shape[2]

    def partial_of(member, q):
        rows = pl.ds(pl.multiple_of(member * rows_out, rows_out), rows_out)
        acts = act_ref[rows, :]
        return jnp.concatenate(
            [
                jnp.dot(acts, og_ref[q * blocks + b], preferred_element_type=jnp.float32)
                for b in range(blocks)
            ],
            axis=1,
        )

    def near_copy(which, q):
        return pltpu.make_async_remote_copy(
            src_ref=near_out.at[which, q],
            dst_ref=near_in.at[which, q],
            send_sem=near_send.at[which, q],
            recv_sem=near_recv.at[which, q],
            device_id=near_id,
            device_id_type=MESH,
        )

    def far_copy(q):
        return pltpu.make_async_remote_copy(
            src_ref=far_out.at[q],
            dst_ref=far_in.at[q],
            send_sem=far_send.at[q],
            recv_sem=far_recv.at[q],
            device_id=far_id,
            device_id_type=MESH,
        )

    def give_near(which, member, q):
        near_out[which, q] = partial_of(member, q).astype(jnp.bfloat16)
        near_copy(which, q).start()

    def give_far(q):
        mine = partial_of(far, q)
        near_copy(0, q).wait_recv()
        far_out[q] = (mine + near_in[0, q].astype(jnp.float32)).astype(jnp.bfloat16)
        far_copy(q).start()

    give_near(0, far_near, 0)
    for q in range(1, parts):
        give_near(0, far_near, q)
        give_far(q - 1)
    give_far(parts - 1)
    for q in range(parts):
        give_near(1, near, q)
    for q in range(parts):
        mine = partial_of(me, q)
        near_copy(1, q).wait_recv()
        mine = mine + near_in[1, q].astype(jnp.float32)
        far_copy(q).wait_recv()
        span = blocks * cols
        out_ref[:, q * span : (q + 1) * span] = (
            mine + far_in[q].astype(jnp.float32)
        ).astype(jnp.bfloat16)
    for q in range(parts):
        near_copy(0, q).wait_send()
        near_copy(1, q).wait_send()
        far_copy(q).wait_send()


def mix_and_scatter(acts, og):
    n, _, cols = og.shape
    parts = math.gcd(n, 4)
    rows_out = acts.shape[0] // 4
    span = n // parts * cols
    vmem = pl.BlockSpec(memory_space=pltpu.VMEM)
    return pl.pallas_call(
        functools.partial(mix_kernel, parts),
        out_shape=jax.ShapeDtypeStruct((rows_out, n * cols), jnp.bfloat16),
        in_specs=[vmem] * 2,
        out_specs=vmem,
        scratch_shapes=[
            pltpu.VMEM((2, parts, rows_out, span), jnp.bfloat16),
            pltpu.VMEM((2, parts, rows_out, span), jnp.bfloat16),
            pltpu.VMEM((parts, rows_out, span), jnp.bfloat16),
            pltpu.VMEM((parts, rows_out, span), jnp.bfloat16),
            pltpu.SemaphoreType.DMA((2, parts)),
            pltpu.SemaphoreType.DMA((2, parts)),
            pltpu.SemaphoreType.DMA((parts,)),
            pltpu.SemaphoreType.DMA((parts,)),
        ],
        compiler_params=pltpu.CompilerParams(
            collective_id=1, has_side_effects=True, vmem_limit_bytes=VMEM_GRANT
        ),
        name="mix_scatter",
    )(acts, og)


def plain_shards(
    tokens,
    norm_gain,
    w_query,
    w_key,
    w_value,
    w_content,
    w_gate,
    sink_logit,
    conv_weight,
    conv_bias,
    channel_gain,
    out_attn,
    out_conv,
):
    token_count = tokens.shape[0]
    offset = lax.axis_index("sp") * token_count
    positions = offset + jnp.arange(token_count, dtype=jnp.int32)
    tokens_wide = tokens.astype(jnp.float32)
    inv_rms = lax.rsqrt(jnp.mean(tokens_wide * tokens_wide, axis=1, keepdims=True) + EPS)
    scaled = (tokens_wide * norm_gain[None, :]).astype(jnp.bfloat16)
    widths = [
        w_query.shape[1],
        w_key.shape[1],
        w_value.shape[1],
        w_content.shape[1],
        w_gate.shape[1],
    ]
    whole_weights = (
        lax.all_gather(w_query, "sp", axis=0, tiled=True),
        lax.all_gather(w_key, "sp", axis=0, tiled=True),
        lax.all_gather(w_value, "sp", axis=0, tiled=True),
        lax.all_gather(w_content, "sp", axis=0, tiled=True),
        lax.all_gather(w_gate, "sp", axis=0, tiled=True),
    )
    joined_whole = jnp.concatenate(whole_weights, axis=1)
    projected = jnp.dot(scaled, joined_whole, preferred_element_type=jnp.float32)
    projected = projected * inv_rms
    bounds = [0]
    for width in widths:
        bounds.append(bounds[-1] + width)
    proj_query = projected[:, bounds[0] : bounds[1]]
    proj_key = projected[:, bounds[1] : bounds[2]]
    proj_value = projected[:, bounds[2] : bounds[3]]
    proj_content = projected[:, bounds[3] : bounds[4]]
    proj_gate = projected[:, bounds[4] : bounds[5]]
    kv_local = widths[1] // HEAD_DIM
    heads_local = widths[0] // HEAD_DIM
    group_size = heads_local // kv_local
    queries = rotate(proj_query.reshape(token_count, heads_local, HEAD_DIM), positions).astype(
        jnp.bfloat16
    )
    key_rows = rotate(proj_key.reshape(token_count, kv_local, HEAD_DIM), positions).astype(
        jnp.bfloat16
    )
    value_rows = proj_value.astype(jnp.bfloat16).reshape(token_count, kv_local, HEAD_DIM)
    glu_out = (proj_content * jax.nn.sigmoid(proj_gate)).astype(jnp.bfloat16)
    prior_key, prior_value, prior_glu = shifted(
        (
            key_rows[token_count - WINDOW :],
            value_rows[token_count - WINDOW :],
            glu_out[token_count - (KERNEL - 1) :],
        ),
        "sp",
        1,
    )
    key_ext = jnp.concatenate([prior_key, key_rows], 0)
    value_ext = jnp.concatenate([prior_value, value_rows], 0)
    block_rows = math.gcd(token_count, 512)
    sink_col = sink_logit.reshape(kv_local, group_size)[:, :, None, None]

    def attend(block_start):
        query_blk = lax.dynamic_slice_in_dim(queries, block_start, block_rows, 0).reshape(
            block_rows, kv_local, group_size, HEAD_DIM
        )
        key_blk = lax.dynamic_slice_in_dim(key_ext, block_start, block_rows + WINDOW, 0)
        value_blk = lax.dynamic_slice_in_dim(value_ext, block_start, block_rows + WINDOW, 0)
        scores = jnp.einsum(
            "qkgd,jkd->kgqj", query_blk, key_blk, preferred_element_type=jnp.float32
        ) * HEAD_DIM ** (-0.5)
        query_pos = offset + block_start + jnp.arange(block_rows, dtype=jnp.int32)
        key_pos = offset + block_start - WINDOW + jnp.arange(block_rows + WINDOW, dtype=jnp.int32)
        distance = query_pos[:, None] - key_pos[None, :]
        allowed = (distance >= 0) & (distance < WINDOW) & (key_pos[None, :] >= 0)
        scores = jnp.where(allowed[None, None], scores, -1e30)
        row_max = jnp.maximum(jnp.max(scores, axis=-1, keepdims=True), sink_col)
        weights = jnp.exp(scores - row_max)
        denominator = jnp.sum(weights, axis=-1, keepdims=True) + jnp.exp(sink_col - row_max)
        probability = (weights / denominator).astype(jnp.bfloat16)
        attended = jnp.einsum(
            "kgqj,jkd->qkgd", probability, value_blk, preferred_element_type=jnp.float32
        )
        return attended.reshape(block_rows, heads_local * HEAD_DIM).astype(jnp.bfloat16)

    starts = jnp.arange(0, token_count, block_rows, dtype=jnp.int32)
    attn_out = lax.map(attend, starts).reshape(token_count, heads_local * HEAD_DIM)
    padded = jnp.concatenate([prior_glu, glu_out], 0)
    conv_sum = jnp.zeros(glu_out.shape, jnp.float32) + conv_bias[None, :]
    for tap_index in range(KERNEL):
        window_rows = lax.slice_in_dim(padded, tap_index, tap_index + token_count, axis=0)
        conv_sum = conv_sum + conv_weight[tap_index][None, :] * window_rows.astype(jnp.float32)
    row_sum, row_squares = lax.psum(
        (jnp.sum(conv_sum, axis=1), jnp.sum(conv_sum * conv_sum, axis=1)), "tp"
    )
    centre = row_sum / CONV_CH
    variance = jnp.maximum(row_squares / CONV_CH - centre * centre, 0.0)
    centred = conv_sum - centre[:, None]
    conv_out = jax.nn.silu(
        centred * lax.rsqrt(variance + EPS)[:, None] * channel_gain[None, :]
    ).astype(jnp.bfloat16)
    attn_weight, conv_weight_out = (
        lax.all_gather(out_attn, "sp", axis=1, tiled=True),
        lax.all_gather(out_conv, "sp", axis=1, tiled=True),
    )
    return lax.psum_scatter(
        (
            jnp.dot(attn_out, attn_weight, preferred_element_type=jnp.float32)
            + jnp.dot(conv_out, conv_weight_out, preferred_element_type=jnp.float32)
        ).astype(jnp.bfloat16),
        "tp",
        scatter_dimension=0,
        tiled=True,
    )


def ring_shards(
    tokens,
    norm_gain,
    w_query,
    w_key,
    w_value,
    w_content,
    w_gate,
    sink_logit,
    conv_weight,
    conv_bias,
    channel_gain,
    out_attn,
    out_conv,
):
    token_count = tokens.shape[0]
    offset = lax.axis_index("sp") * token_count
    positions = offset + jnp.arange(token_count, dtype=jnp.int32)
    w_own = jnp.concatenate([w_query, w_key, w_value, w_content, w_gate], axis=1)
    o_own = jnp.concatenate([out_attn, out_conv], axis=0)
    lane = jnp.arange(LANES, dtype=jnp.int32)
    half_dim = HEAD_DIM // 2
    inverse = 1.0 / THETA ** ((lane % half_dim).astype(jnp.float32) * 2.0 / HEAD_DIM)
    angles = positions.astype(jnp.float32)[:, None] * inverse[None, :]
    sign = jnp.where(lane % HEAD_DIM < half_dim, -1.0, 1.0)
    acts, mix_weight = gather_and_mix(
        lax.axis_size("sp"), tokens, norm_gain, w_own, o_own,
        jnp.cos(angles), jnp.sin(angles) * sign[None, :],
        sink_logit, conv_weight, conv_bias, channel_gain,
    )
    return mix_and_scatter(acts, mix_weight)


def solution(mesh):
    placed = (
        P("sp", None),
        P(),
        P("sp", "tp"),
        P("sp", "tp"),
        P("sp", "tp"),
        P("sp", "tp"),
        P("sp", "tp"),
        P("tp"),
        P(None, "tp"),
        P("tp"),
        P("tp"),
        P("tp", "sp"),
        P("tp", "sp"),
    )
    sp, tp = mesh.shape["sp"], mesh.shape["tp"]
    ringed = tp == 4 and sp % 2 == 0

    def shards(*arrays):
        fits = (
            ringed
            and arrays[11].shape[1] % LANES == 0
            and arrays[2].shape[0] % LANES == 0
            and arrays[0].shape[0] % (WINDOW * tp) == 0
            and arrays[2].shape[1] % LANES == 0
            and arrays[3].shape[1] == HEAD_DIM
            and arrays[5].shape[1] % LANES == 0
        )
        return (ring_shards if fits else plain_shards)(*arrays)

    return jax.shard_map(
        shards, mesh=mesh, in_specs=placed, out_specs=P(("sp", "tp"), None), check_vma=False
    )
```

```python
import functools
import math

import jax
import jax.numpy as jnp
from jax import lax
from jax.experimental import pallas as pl
from jax.experimental.pallas import tpu as pltpu
from jax.sharding import PartitionSpec as P

HEAD_DIM = 64
CONV_CH = 1024
KERNEL = 31
WINDOW = 128


EPS = 1e-05
THETA = 10000.0


def shifted(block, axis, distance):
    devices = range(lax.axis_size(axis))
    route = [(i - distance, i) for i in devices if i - distance in devices]
    return lax.ppermute(block, axis, route)


def rotate(heads_in, positions):
    half_dim = heads_in.shape[-1] // 2
    inverse = 1.0 / THETA ** (jnp.arange(half_dim, dtype=jnp.float32) * 2.0 / heads_in.shape[-1])
    angles = positions.astype(jnp.float32)[:, None] * inverse[None, :]
    cosine = jnp.cos(angles)[:, None, :]
    sine_part = jnp.sin(angles)[:, None, :]
    former = heads_in[..., :half_dim]
    latter = heads_in[..., half_dim:]
    return jnp.concatenate(
        [former * cosine - latter * sine_part, latter * cosine + former * sine_part], axis=-1
    )


MESH = pl.DeviceIdType.MESH
LANES = 128
VMEM_GRANT = 60 * 1024 * 1024


def ring_place(index, n):
    odd = index % 2
    return (index // 2) * (1 - odd) + (n - 1 - index // 2) * odd


def ring_member(place, n):
    return jnp.where(place < (n + 1) // 2, 2 * place, 2 * (n - 1 - place) + 1)


def greet(peers):
    barrier = pltpu.get_barrier_semaphore()
    for peer in peers:
        pl.semaphore_signal(barrier, inc=1, device_id=peer, device_id_type=MESH)
    pl.semaphore_wait(barrier, len(peers))


def project_kernel(
    n, pieces, head_lanes,
    tok_ref, gain_ref, w_ref, oa_ref, oc_ref, cos_ref, sin_ref, far_cos_ref, far_sin_ref,
    sink_ref, taps_ref, bias_ref, chan_ref, out_ref, act_ref, og_ref,
    near_out, near_in, far_out, far_in,
    scaled, inv, wg, proj_ref, turned, key_ext, value_ext, glu_ext, conv, stats, peer_stats,
    w_send, w_recv, o_send, o_recv, halo_send, halo_recv, stat_send, stat_recv,
    near_send, near_recv, far_send, far_recv,
):
    me = lax.axis_index("sp")
    place = ring_place(me, n)
    after = {"sp": ring_member(lax.rem(place + 1, n), n)}
    before = {"sp": ring_member(lax.rem(place + n - 1, n), n)}
    following = {"sp": lax.rem(me + 1, n)}
    previous = {"sp": lax.rem(me + n - 1, n)}
    members = lax.axis_size("tp")
    mine_tp = lax.axis_index("tp")
    siblings = [{"tp": lax.rem(mine_tp + k, members)} for k in range(1, members)]
    greet([after, before, following, previous] + siblings)

    def hop(own, own_start, held, send, recv, d, c, s):
        half = held.shape[1] // 2
        sub = half // pieces
        rows = pl.ds(d * half + c * sub, sub)
        offset = n - s if d == 0 else s
        owner = ring_member(lax.rem(place + offset, n), n)
        return pltpu.make_async_remote_copy(
            src_ref=own.at[pl.ds(own_start + c * sub, sub)] if s == 0 else held.at[owner, rows],
            dst_ref=held.at[owner, rows],
            send_sem=send.at[d, s, c],
            recv_sem=recv.at[d, s, c],
            device_id=after if d == 0 else before,
            device_id_type=MESH,
        )

    def w_hop(d, c, s):
        return hop(w_ref, d * (w_ref.shape[0] // 2), wg, w_send, w_recv, d, c, s)

    def o_hop(d, c, s):
        return hop(oc_ref if d else oa_ref, 0, og_ref, o_send, o_recv, d, c, s)

    lanes = [(d, c) for c in range(pieces) for d in range(2)]
    for d, c in lanes:
        w_hop(d, c, 0).start()

    token_count, width = tok_ref.shape
    depth = w_ref.shape[0]
    step_rows = math.gcd(token_count, 64)

    @pl.loop(0, token_count // step_rows)
    def _(i):
        rows = pl.ds(pl.multiple_of(i * step_rows, step_rows), step_rows)
        wide = tok_ref[rows, :].astype(jnp.float32)
        inv[rows, :] = lax.rsqrt(jnp.sum(wide * wide, axis=1, keepdims=True) / width + EPS)
        scaled[rows, :] = (wide * gain_ref[...]).astype(jnp.bfloat16)

    tile = math.gcd(token_count, 256)
    attn_rows = oa_ref.shape[0]
    og_ref[me, 0:attn_rows] = oa_ref[...]
    og_ref[me, attn_rows:] = oc_ref[...]

    def add(terms, first, last):
        @pl.loop(0, token_count // tile)
        def _(i):
            rows = pl.ds(pl.multiple_of(i * tile, tile), tile)
            total = None if first else proj_ref[rows, :]
            for owner, block in terms:
                columns = pl.ds(pl.multiple_of(owner * depth, depth), depth)
                term = jnp.dot(
                    scaled[rows, columns], block(), preferred_element_type=jnp.float32
                )
                total = term if total is None else total + term
            proj_ref[rows, :] = total * inv[rows, :] if last else total

    add([(me, lambda: w_ref[...])], True, n == 1)
    for t in range(n - 1):
        for d, c in lanes:
            w_hop(d, c, t).wait_recv()
            if t < n - 2:
                w_hop(d, c, t + 1).start()
        if t == max(n - 3, 0):
            for d, c in lanes:
                o_hop(d, c, 0).start()
        ready = [k for k in range(1, n) if max(k, n - k) - 1 == t]
        if ready:
            owners = [ring_member(lax.rem(place + n - k, n), n) for k in ready]
            add([(o, lambda o=o: wg[o]) for o in owners], False, t == n - 2)

    def o_advance(t):
        if t >= n - 1:
            return
        for d, c in lanes:
            o_hop(d, c, t).wait_recv()
            if t < n - 2:
                o_hop(d, c, t + 1).start()

    head_w = LANES // 2
    channels = taps_ref.shape[1]
    at_glu = head_lanes + LANES
    lead = glu_ext.shape[0] - token_count
    tiles = token_count // WINDOW

    def lane_of(shape):
        return lax.broadcasted_iota(jnp.int32, shape, 1)

    def turn(x, cosine, sine_part):
        low = lane_of(x.shape) % head_w < head_w // 2
        swapped = jnp.where(
            low, pltpu.roll(x, LANES - head_w // 2, 1), pltpu.roll(x, head_w // 2, 1)
        )
        return x * cosine + jnp.where(low, -swapped, swapped) * sine_part

    def shape_rows(i):
        base = pl.multiple_of(i * WINDOW, WINDOW)
        rows = pl.ds(base, WINDOW)
        near_cos, near_sin = cos_ref[...], sin_ref[...]
        far_cos, far_sin = far_cos_ref[pl.ds(i, 1), :], far_sin_ref[pl.ds(i, 1), :]
        cosine = near_cos * far_cos - near_sin * far_sin
        sine_part = near_sin * far_cos + near_cos * far_sin
        for start in range(0, head_lanes, LANES):
            cut = slice(start, start + LANES)
            turned[rows, cut] = turn(proj_ref[rows, cut], cosine, sine_part).astype(jnp.bfloat16)
        pair = proj_ref[rows, head_lanes:at_glu]
        key_part = turn(pair, cosine, sine_part)
        low = lane_of(pair.shape) < head_w
        ext = pl.ds(base + WINDOW, WINDOW)
        key_ext[ext, :] = jnp.where(low, key_part, pltpu.roll(key_part, head_w, 1)).astype(
            jnp.bfloat16
        )
        value_ext[ext, :] = jnp.where(low, pltpu.roll(pair, head_w, 1), pair).astype(jnp.bfloat16)
        content = proj_ref[rows, at_glu : at_glu + channels]
        gate = proj_ref[rows, at_glu + channels : at_glu + 2 * channels]
        glu_ext[pl.ds(base + lead, WINDOW), :] = (
            (content * jax.nn.sigmoid(gate)).astype(jnp.bfloat16).astype(jnp.float32)
        )

    pl.loop(0, tiles)(shape_rows)

    def halo(which):
        ref, count = ((key_ext, WINDOW), (value_ext, WINDOW), (glu_ext, lead))[which]
        return pltpu.make_async_remote_copy(
            src_ref=ref.at[pl.ds(token_count, count)],
            dst_ref=ref.at[pl.ds(0, count)],
            send_sem=halo_send.at[which],
            recv_sem=halo_recv.at[which],
            device_id=following,
            device_id_type=MESH,
        )

    for which in range(3):
        halo(which).start()

    def convolve(i):
        base = pl.multiple_of(i * WINDOW, WINDOW)
        shift = lead - (KERNEL - 1)
        row_sum = row_squares = None
        for start in range(0, channels, LANES):
            cut = slice(start, start + LANES)
            parts = []
            for sub in range(0, WINDOW, 64):
                slab = glu_ext[pl.ds(base + sub, 64 + lead), cut]
                total = jnp.zeros((64, LANES), jnp.float32) + bias_ref[:, cut]
                for r in range(8):
                    moved = slab if r == 0 else pltpu.roll(slab, 64 + lead - r, 0)
                    for m in range(0, lead + 1, 8):
                        tap = m + r - shift
                        if 0 <= tap < KERNEL:
                            total = total + taps_ref[tap : tap + 1, cut] * moved[m : m + 64]
                parts.append(total)
            summed = jnp.concatenate(parts, axis=0)
            conv[pl.ds(base, WINDOW), cut] = summed
            one = jnp.sum(summed, axis=1, keepdims=True)
            two = jnp.sum(summed * summed, axis=1, keepdims=True)
            row_sum = one if row_sum is None else row_sum + one
            row_squares = two if row_squares is None else row_squares + two
        lane = lane_of((WINDOW, LANES))
        packed = jnp.where(lane == 0, row_sum, jnp.where(lane == 1, row_squares, 0.0))
        stats[:, pl.ds(base, WINDOW)] = packed.T[:8, :]

    half_tiles = max(tiles // 2, 1)
    pl.loop(1, half_tiles)(convolve)
    o_advance(0)
    pl.loop(half_tiles, tiles)(convolve)
    halo(2).wait_recv()
    glu_ext[0:lead, :] = jnp.where(me > 0, glu_ext[0:lead, :], 0.0)
    convolve(0)

    def stat_copy(k):
        return pltpu.make_async_remote_copy(
            src_ref=stats,
            dst_ref=peer_stats.at[k],
            send_sem=stat_send.at[k],
            recv_sem=stat_recv.at[k],
            device_id=siblings[k],
            device_id_type=MESH,
        )

    for k in range(members - 1):
        stat_copy(k).start()
    o_advance(1)

    def attend(i):
        base = pl.multiple_of(i * WINDOW, WINDOW)
        rows, reach = pl.ds(base, WINDOW), pl.ds(base, 2 * WINDOW)
        keys, values = key_ext[reach, :], value_ext[reach, :]
        shape = (WINDOW, 2 * WINDOW)
        column = lane_of(shape)
        distance = lax.broadcasted_iota(jnp.int32, shape, 0) - column + WINDOW
        first = me * token_count + i * WINDOW - WINDOW
        allowed = (distance >= 0) & (distance < WINDOW) & (column + first >= 0)
        low = lane_of((WINDOW, LANES)) < head_w
        for start in range(0, head_lanes, LANES):
            cut = slice(start, start + LANES)
            both = turned[rows, cut].astype(jnp.float32)
            found = []
            for side in range(2):
                sink = sink_ref[start // head_w + side]
                query = jnp.where(low if side == 0 else ~low, both, 0.0).astype(jnp.bfloat16)
                scores = lax.dot_general(
                    query, keys, (((1,), (1,)), ((), ())), preferred_element_type=jnp.float32
                ) * HEAD_DIM ** (-0.5)
                scores = jnp.where(allowed, scores, -1e30)
                row_max = jnp.maximum(jnp.max(scores, axis=1, keepdims=True), sink)
                weights = jnp.exp(scores - row_max)
                denominator = jnp.sum(weights, axis=1, keepdims=True) + jnp.exp(sink - row_max)
                probability = (weights * (1.0 / denominator)).astype(jnp.bfloat16)
                found.append(jnp.dot(probability, values, preferred_element_type=jnp.float32))
            act_ref[rows, cut] = jnp.where(low, found[0], found[1]).astype(jnp.bfloat16)

    pl.loop(1, half_tiles)(attend)
    o_advance(2)
    pl.loop(half_tiles, tiles)(attend)
    halo(0).wait_recv()
    halo(1).wait_recv()
    attend(0)
    o_advance(3)
    for k in range(members - 1):
        stat_copy(k).wait_recv()

    def normalise(i):
        base = pl.multiple_of(i * WINDOW, WINDOW)
        rows = pl.ds(base, WINDOW)
        total = stats[:, rows]
        for k in range(members - 1):
            total = total + peer_stats[k, :, rows]
        total = total * (1.0 / (channels * members))
        column = jnp.concatenate([total] * (LANES // 8), axis=0).T
        centre = column[:, 0:1]
        variance = jnp.maximum(column[:, 1:2] - centre * centre, 0.0)
        normed = (conv[rows, :] - centre) * lax.rsqrt(variance + EPS) * chan_ref[...]
        act_ref[rows, head_lanes : head_lanes + channels] = (
            normed * jax.nn.sigmoid(normed)
        ).astype(jnp.bfloat16)

    pl.loop(0, tiles)(normalise)

    near = mine_tp + 1 - 2 * (mine_tp % 2)
    far = lax.rem(mine_tp + 2, members)
    far_near = lax.rem(near + 2, members)
    rows_out = out_ref.shape[0]
    cols = oa_ref.shape[1]

    def partial_of(member, owner):
        rows = pl.ds(pl.multiple_of(member * rows_out, rows_out), rows_out)
        return jnp.dot(act_ref[rows, :], og_ref[owner], preferred_element_type=jnp.float32)

    def near_copy(which, q):
        return pltpu.make_async_remote_copy(
            src_ref=near_out.at[which, q],
            dst_ref=near_in.at[which, q],
            send_sem=near_send.at[which, q],
            recv_sem=near_recv.at[which, q],
            device_id={"tp": near},
            device_id_type=MESH,
        )

    def far_copy(q):
        return pltpu.make_async_remote_copy(
            src_ref=far_out.at[q],
            dst_ref=far_in.at[q],
            send_sem=far_send.at[q],
            recv_sem=far_recv.at[q],
            device_id={"tp": far},
            device_id_type=MESH,
        )

    distances = [(0, 0)] + sorted((max(k, n - k), k) for k in range(1, n))
    owners = [ring_member(lax.rem(place + n - k, n), n) for _, k in distances]

    def give_near(which, member, q):
        near_out[which, q] = partial_of(member, owners[q]).astype(jnp.bfloat16)
        near_copy(which, q).start()

    def give_far(q):
        mine = partial_of(far, owners[q])
        near_copy(0, q).wait_recv()
        far_out[q] = (mine + near_in[0, q].astype(jnp.float32)).astype(jnp.bfloat16)
        far_copy(q).start()

    advanced = 4
    for q in range(n):
        waits = advanced < distances[q][0]
        if q > 0 and waits:
            give_far(q - 1)
        while advanced < distances[q][0]:
            o_advance(advanced)
            advanced += 1
        give_near(0, far_near, q)
        if q > 0 and not waits:
            give_far(q - 1)
    give_far(n - 1)
    for q in range(n):
        give_near(1, near, q)
    for q in range(n):
        mine = partial_of(mine_tp, owners[q])
        near_copy(1, q).wait_recv()
        mine = mine + near_in[1, q].astype(jnp.float32)
        far_copy(q).wait_recv()
        span = pl.ds(pl.multiple_of(owners[q] * cols, cols), cols)
        out_ref[:, span] = (mine + far_in[q].astype(jnp.float32)).astype(jnp.bfloat16)
    for q in range(n):
        near_copy(0, q).wait_send()
        near_copy(1, q).wait_send()
        far_copy(q).wait_send()
    for which in range(3):
        halo(which).wait_send()
    for k in range(members - 1):
        stat_copy(k).wait_send()
    for t in range(n - 1):
        for d, c in lanes:
            w_hop(d, c, t).wait_send()
            o_hop(d, c, t).wait_send()


def whole_layer(n, tokens, gain, w_own, oa, oc, tables, sink, taps, bias, chan):
    token_count = tokens.shape[0]
    channels = taps.shape[1]
    head_lanes = sink.shape[0] * HEAD_DIM
    lead = -(-(KERNEL - 1) // 8) * 8
    members = lax.axis_size("tp")
    pieces = 2
    cols = oa.shape[1]
    rows_out = token_count // members
    dma = pltpu.SemaphoreType.DMA
    sems = dma((2, n - 1, pieces))
    vmem = pl.BlockSpec(memory_space=pltpu.VMEM)
    smem = pl.BlockSpec(memory_space=pltpu.SMEM)
    return pl.pallas_call(
        functools.partial(project_kernel, n, pieces, head_lanes),
        out_shape=jax.ShapeDtypeStruct((rows_out, n * cols), jnp.bfloat16),
        in_specs=[vmem] * 9 + [smem] + [vmem] * 3,
        out_specs=vmem,
        scratch_shapes=[
            pltpu.VMEM((token_count, head_lanes + channels), jnp.bfloat16),
            pltpu.VMEM((n, oa.shape[0] + oc.shape[0], cols), jnp.bfloat16),
            pltpu.VMEM((2, n, rows_out, cols), jnp.bfloat16),
            pltpu.VMEM((2, n, rows_out, cols), jnp.bfloat16),
            pltpu.VMEM((n, rows_out, cols), jnp.bfloat16),
            pltpu.VMEM((n, rows_out, cols), jnp.bfloat16),
            pltpu.VMEM(tokens.shape, jnp.bfloat16),
            pltpu.VMEM((token_count, 1), jnp.float32),
            pltpu.VMEM((n,) + w_own.shape, jnp.bfloat16),
            pltpu.VMEM((token_count, w_own.shape[1]), jnp.float32),
            pltpu.VMEM((token_count, head_lanes), jnp.bfloat16),
            pltpu.VMEM((token_count + WINDOW, LANES), jnp.bfloat16),
            pltpu.VMEM((token_count + WINDOW, LANES), jnp.bfloat16),
            pltpu.VMEM((token_count + lead, channels), jnp.float32),
            pltpu.VMEM((token_count, channels), jnp.float32),
            pltpu.VMEM((8, token_count), jnp.float32),
            pltpu.VMEM((members - 1, 8, token_count), jnp.float32),
            sems, sems, sems, sems,
            dma((3,)), dma((3,)), dma((members - 1,)), dma((members - 1,)),
            dma((2, n)), dma((2, n)), dma((n,)), dma((n,)),
        ],
        compiler_params=pltpu.CompilerParams(
            collective_id=0, has_side_effects=True, vmem_limit_bytes=VMEM_GRANT
        ),
        name="whole_layer",
    )(
        tokens, gain[None, :], w_own, oa, oc, *tables, sink, taps,
        bias[None, :], chan[None, :],
    )


def plain_shards(
    tokens,
    norm_gain,
    w_query,
    w_key,
    w_value,
    w_content,
    w_gate,
    sink_logit,
    conv_weight,
    conv_bias,
    channel_gain,
    out_attn,
    out_conv,
):
    token_count = tokens.shape[0]
    offset = lax.axis_index("sp") * token_count
    positions = offset + jnp.arange(token_count, dtype=jnp.int32)
    tokens_wide = tokens.astype(jnp.float32)
    inv_rms = lax.rsqrt(jnp.mean(tokens_wide * tokens_wide, axis=1, keepdims=True) + EPS)
    scaled = (tokens_wide * norm_gain[None, :]).astype(jnp.bfloat16)
    widths = [
        w_query.shape[1],
        w_key.shape[1],
        w_value.shape[1],
        w_content.shape[1],
        w_gate.shape[1],
    ]
    whole_weights = (
        lax.all_gather(w_query, "sp", axis=0, tiled=True),
        lax.all_gather(w_key, "sp", axis=0, tiled=True),
        lax.all_gather(w_value, "sp", axis=0, tiled=True),
        lax.all_gather(w_content, "sp", axis=0, tiled=True),
        lax.all_gather(w_gate, "sp", axis=0, tiled=True),
    )
    joined_whole = jnp.concatenate(whole_weights, axis=1)
    projected = jnp.dot(scaled, joined_whole, preferred_element_type=jnp.float32)
    projected = projected * inv_rms
    bounds = [0]
    for width in widths:
        bounds.append(bounds[-1] + width)
    proj_query = projected[:, bounds[0] : bounds[1]]
    proj_key = projected[:, bounds[1] : bounds[2]]
    proj_value = projected[:, bounds[2] : bounds[3]]
    proj_content = projected[:, bounds[3] : bounds[4]]
    proj_gate = projected[:, bounds[4] : bounds[5]]
    kv_local = widths[1] // HEAD_DIM
    heads_local = widths[0] // HEAD_DIM
    group_size = heads_local // kv_local
    queries = rotate(proj_query.reshape(token_count, heads_local, HEAD_DIM), positions).astype(
        jnp.bfloat16
    )
    key_rows = rotate(proj_key.reshape(token_count, kv_local, HEAD_DIM), positions).astype(
        jnp.bfloat16
    )
    value_rows = proj_value.astype(jnp.bfloat16).reshape(token_count, kv_local, HEAD_DIM)
    glu_out = (proj_content * jax.nn.sigmoid(proj_gate)).astype(jnp.bfloat16)
    prior_key, prior_value, prior_glu = shifted(
        (
            key_rows[token_count - WINDOW :],
            value_rows[token_count - WINDOW :],
            glu_out[token_count - (KERNEL - 1) :],
        ),
        "sp",
        1,
    )
    key_ext = jnp.concatenate([prior_key, key_rows], 0)
    value_ext = jnp.concatenate([prior_value, value_rows], 0)
    block_rows = math.gcd(token_count, 512)
    sink_col = sink_logit.reshape(kv_local, group_size)[:, :, None, None]

    def attend(block_start):
        query_blk = lax.dynamic_slice_in_dim(queries, block_start, block_rows, 0).reshape(
            block_rows, kv_local, group_size, HEAD_DIM
        )
        key_blk = lax.dynamic_slice_in_dim(key_ext, block_start, block_rows + WINDOW, 0)
        value_blk = lax.dynamic_slice_in_dim(value_ext, block_start, block_rows + WINDOW, 0)
        scores = jnp.einsum(
            "qkgd,jkd->kgqj", query_blk, key_blk, preferred_element_type=jnp.float32
        ) * HEAD_DIM ** (-0.5)
        query_pos = offset + block_start + jnp.arange(block_rows, dtype=jnp.int32)
        key_pos = offset + block_start - WINDOW + jnp.arange(block_rows + WINDOW, dtype=jnp.int32)
        distance = query_pos[:, None] - key_pos[None, :]
        allowed = (distance >= 0) & (distance < WINDOW) & (key_pos[None, :] >= 0)
        scores = jnp.where(allowed[None, None], scores, -1e30)
        row_max = jnp.maximum(jnp.max(scores, axis=-1, keepdims=True), sink_col)
        weights = jnp.exp(scores - row_max)
        denominator = jnp.sum(weights, axis=-1, keepdims=True) + jnp.exp(sink_col - row_max)
        probability = (weights / denominator).astype(jnp.bfloat16)
        attended = jnp.einsum(
            "kgqj,jkd->qkgd", probability, value_blk, preferred_element_type=jnp.float32
        )
        return attended.reshape(block_rows, heads_local * HEAD_DIM).astype(jnp.bfloat16)

    starts = jnp.arange(0, token_count, block_rows, dtype=jnp.int32)
    attn_out = lax.map(attend, starts).reshape(token_count, heads_local * HEAD_DIM)
    padded = jnp.concatenate([prior_glu, glu_out], 0)
    conv_sum = jnp.zeros(glu_out.shape, jnp.float32) + conv_bias[None, :]
    for tap_index in range(KERNEL):
        window_rows = lax.slice_in_dim(padded, tap_index, tap_index + token_count, axis=0)
        conv_sum = conv_sum + conv_weight[tap_index][None, :] * window_rows.astype(jnp.float32)
    row_sum, row_squares = lax.psum(
        (jnp.sum(conv_sum, axis=1), jnp.sum(conv_sum * conv_sum, axis=1)), "tp"
    )
    centre = row_sum / CONV_CH
    variance = jnp.maximum(row_squares / CONV_CH - centre * centre, 0.0)
    centred = conv_sum - centre[:, None]
    conv_out = jax.nn.silu(
        centred * lax.rsqrt(variance + EPS)[:, None] * channel_gain[None, :]
    ).astype(jnp.bfloat16)
    attn_weight, conv_weight_out = (
        lax.all_gather(out_attn, "sp", axis=1, tiled=True),
        lax.all_gather(out_conv, "sp", axis=1, tiled=True),
    )
    return lax.psum_scatter(
        (
            jnp.dot(attn_out, attn_weight, preferred_element_type=jnp.float32)
            + jnp.dot(conv_out, conv_weight_out, preferred_element_type=jnp.float32)
        ).astype(jnp.bfloat16),
        "tp",
        scatter_dimension=0,
        tiled=True,
    )


def ring_shards(
    tokens,
    norm_gain,
    w_query,
    w_key,
    w_value,
    w_content,
    w_gate,
    sink_logit,
    conv_weight,
    conv_bias,
    channel_gain,
    out_attn,
    out_conv,
):
    token_count = tokens.shape[0]
    offset = lax.axis_index("sp") * token_count
    positions = offset + jnp.arange(token_count, dtype=jnp.int32)
    w_own = jnp.concatenate([w_query, w_key, w_value, w_content, w_gate], axis=1)
    half_dim = HEAD_DIM // 2
    lane = jnp.arange(LANES, dtype=jnp.int32)
    inverse = 1.0 / THETA ** ((lane % half_dim).astype(jnp.float32) * 2.0 / HEAD_DIM)
    near_angle = jnp.arange(WINDOW, dtype=jnp.float32)[:, None] * inverse[None, :]
    far_angle = positions[::WINDOW].astype(jnp.float32)[:, None] * inverse[None, :]
    tables = (jnp.cos(near_angle), jnp.sin(near_angle), jnp.cos(far_angle), jnp.sin(far_angle))
    return whole_layer(
        lax.axis_size("sp"), tokens, norm_gain, w_own, out_attn, out_conv, tables,
        sink_logit, conv_weight, conv_bias, channel_gain,
    )


def solution(mesh):
    placed = (
        P("sp", None),
        P(),
        P("sp", "tp"),
        P("sp", "tp"),
        P("sp", "tp"),
        P("sp", "tp"),
        P("sp", "tp"),
        P("tp"),
        P(None, "tp"),
        P("tp"),
        P("tp"),
        P("tp", "sp"),
        P("tp", "sp"),
    )
    sp, tp = mesh.shape["sp"], mesh.shape["tp"]
    ringed = tp == 4 and sp % 2 == 0 and sp >= 6

    def shards(*arrays):
        fits = (
            ringed
            and arrays[11].shape[1] % LANES == 0
            and arrays[2].shape[0] % LANES == 0
            and arrays[0].shape[0] % (WINDOW * tp) == 0
            and arrays[2].shape[1] % LANES == 0
            and arrays[3].shape[1] == HEAD_DIM
            and arrays[11].shape[0] == arrays[12].shape[0]
            and arrays[5].shape[1] % LANES == 0
        )
        return (ring_shards if fits else plain_shards)(*arrays)

    return jax.shard_map(
        shards, mesh=mesh, in_specs=placed, out_specs=P(("sp", "tp"), None), check_vma=False
    )
```
